512 devices in a mesh: tp: 32 (over z, core), dp: 16 (over y, x).
Axes of the slice: x: 4, y: 4, z: 16, core: 2. Of those that a mesh axis runs over, the one named last changes fastest.
Arguments:
- tokens: bfloat16 [128, 4096], P('tp', 'dp'), may hold values from -6 to 6
- norm_gain: bfloat16 [2, 4096], P(None, 'dp'), may hold values from 0.099609375 to 1.8984375
- w_query: bfloat16 [2, 4096, 4096], P(None, 'dp', 'tp'), may hold values from -0.09375 to 0.09375
- w_key: bfloat16 [2, 4096, 4096], P(None, 'dp', 'tp'), may hold values from -0.09375 to 0.09375
- w_value: bfloat16 [2, 4096, 4096], P(None, 'dp', 'tp'), may hold values from -0.09375 to 0.09375
- w_outgate: bfloat16 [2, 4096, 4096], P(None, 'dp', 'tp'), may hold values from -0.09375 to 0.09375
- w_gates: bfloat16 [2, 4096, 64], P(None, 'dp'), may hold values from -0.09375 to 0.09375
- gate_bias: float32 [2, 2, 32], P(None, None, 'tp'), may hold values from -1 to 5
- w_out: bfloat16 [2, 4096, 4096], P(None, 'tp', 'dp'), may hold values from -0.09375 to 0.09375
- memory: float32 [2, 128, 32, 128, 128], P(None, 'dp', 'tp'), may hold values from -6 to 6
- normalizer: float32 [2, 128, 32, 128], P(None, 'dp', 'tp'), may hold values from -3 to 3
- stabilizer: float32 [2, 128, 32], P(None, 'dp', 'tp'), may hold values from -8 to 300, as said below
Outputs:
- mixed: bfloat16 [128, 4096], P('tp', 'dp')
- new_memory: float32 [2, 128, 32, 128, 128], P(None, 'dp', 'tp')
- new_normalizer: float32 [2, 128, 32, 128], P(None, 'dp', 'tp')
- new_stabilizer: float32 [2, 128, 32], P(None, 'dp', 'tp')
The draws below stay inside these ranges and needn't reach their ends.
Inputs may be any that keep to these rules, and one draw needn't show every extreme that they name: `stabilizer`: lies between -8 and 8, except that some entries may be as large as 300.
All inputs are finite; a program needn't handle non-finite values.
Results may differ from the reference program's by a relative error of at most 0.04.
Values may be sent and summed in bfloat16 or wider, within the bound.
A program may use at most 64 MiB of HBM per device.

```python
import jax
import jax.numpy as jnp
from jax import lax

D = 4096
HEAD_SIZE = 128
HEADS = 32
SEQS = 128


def draw_stabilizer(key, part):
    shape = (2, SEQS, HEADS)
    values = jnp.clip(2.0 * jax.random.normal(jax.random.fold_in(key, 11), shape, jnp.float32), -8.0, 8.0)
    return values


def shard_levels(own_key, dims, shards, least, high):
    factor_of, own = 1.0, jax.random.fold_in(own_key, 6)
    for dim, shards_of in shards:
        draws = jnp.exp(jax.random.uniform(jax.random.fold_in(own, dim), (shards_of,), jnp.float32, least / len(shards), high / len(shards)))
        factor_of = factor_of * jnp.repeat(draws, dims[dim] // shards_of).reshape([-1 if axis == dim else 1 for axis in range(len(dims))])
    return factor_of


def scatter_about(key, dims, deviation, most, shards=(), held_as=jnp.bfloat16):
    drawn = jax.random.normal(key, dims, jnp.float32) * deviation
    if len(shards) > 0:
        drawn = shard_levels(key, dims, shards, -0.22, 0.18) * drawn
    return jnp.clip(drawn, min=-most, max=most).astype(held_as)


def setup_inputs(seed: int = 0) -> dict:
    splits = jax.random.split(jax.random.key(seed), 13)
    return {
        "tokens": scatter_about(splits[0], (SEQS, D), 1.0, 6.0, ((0, 32), (1, 16))),
        "norm_gain": jnp.clip(1.0 + 0.18 * jax.random.normal(splits[1], (2, D), jnp.float32), 0.099609375, 1.8984375).astype(jnp.bfloat16),
        "w_query": scatter_about(splits[2], (2, D, HEADS * HEAD_SIZE), D ** -0.5, 0.09375, ((1, 16), (2, 32))),
        "w_key": scatter_about(splits[3], (2, D, HEADS * HEAD_SIZE), D ** -0.5, 0.09375, ((1, 16), (2, 32))),
        "w_value": scatter_about(splits[4], (2, D, HEADS * HEAD_SIZE), D ** -0.5, 0.09375, ((1, 16), (2, 32))),
        "w_outgate": scatter_about(splits[5], (2, D, HEADS * HEAD_SIZE), D ** -0.5, 0.09375, ((1, 16), (2, 32))),
        "w_gates": scatter_about(splits[6], (2, D, 2 * HEADS), D ** -0.5, 0.09375, ((1, 16),)),
        "gate_bias": jnp.clip(-1.0 + 6.0 * jax.random.uniform(splits[7], (2, 2, HEADS), jnp.float32) ** shard_levels(splits[7], (2, 2, HEADS), ((2, 32),), -0.2, 0.2), -1.0, 5.0),
        "w_out": scatter_about(splits[8], (2, HEADS * HEAD_SIZE, D), (HEADS * HEAD_SIZE) ** -0.5, 0.09375, ((1, 32), (2, 16))),
        "memory": scatter_about(splits[9], (2, SEQS, HEADS, HEAD_SIZE, HEAD_SIZE), 1.0, 6.0, ((1, 16), (2, 32)), jnp.float32),
        "normalizer": scatter_about(splits[10], (2, SEQS, HEADS, HEAD_SIZE), 0.5, 3.0, ((1, 16), (2, 32)), jnp.float32),
        "stabilizer": draw_stabilizer(jax.random.fold_in(splits[12], 71), 0),
    }


epsilon = 1e-06

def cell_update(query, key_rows, value_rows, input_pre, forget_pre, memory, normalizer, stabilizer):
    batch_size = query.shape[0]
    head_count = input_pre.shape[1]
    query_float = query.astype(jnp.float32).reshape(batch_size, head_count, -1)
    key_float = key_rows.astype(jnp.float32).reshape(batch_size, head_count, -1) * query_float.shape[2] ** (-0.5)
    value_float = value_rows.astype(jnp.float32).reshape(batch_size, head_count, -1)
    carried = jax.nn.log_sigmoid(forget_pre) + stabilizer
    new_max = jnp.maximum(carried, input_pre)
    keep_factor = jnp.exp(carried - new_max)
    write_factor = jnp.exp(input_pre - new_max)
    new_memory = keep_factor[:, :, None, None] * memory + write_factor[:, :, None, None] * value_float[:, :, :, None] * key_float[:, :, None, :]
    new_normalizer = keep_factor[:, :, None] * normalizer + write_factor[:, :, None] * key_float
    numerator = lax.optimization_barrier(jnp.sum(new_memory * query_float[:, :, None, :], axis=3))
    denominator = lax.optimization_barrier(jnp.sum(new_normalizer * query_float, axis=2))
    floor_value = jnp.maximum(jnp.abs(denominator), jnp.exp(-new_max))
    readout = numerator / jnp.maximum(floor_value, 1.0)[:, :, None]
    return (readout.reshape(batch_size, -1), new_memory, new_normalizer, new_max)

def reference(tokens, norm_gain, w_query, w_key, w_value, w_outgate, w_gates, gate_bias, w_out, memory, normalizer, stabilizer):
    current = tokens
    memories = []
    normalizers = []
    maxima = []
    for layer_index in range(2):
        wide_rows = current.astype(jnp.float32)
        inv_scale = lax.rsqrt(lax.optimization_barrier(jnp.sum(wide_rows * wide_rows, axis=1)) / D + epsilon)[:, None]
        scaled = (wide_rows * norm_gain[layer_index].astype(jnp.float32)[None, :]).astype(jnp.bfloat16)
        query = (jnp.dot(scaled, w_query[layer_index], preferred_element_type=jnp.float32) * inv_scale).astype(jnp.bfloat16)
        key_rows = (jnp.dot(scaled, w_key[layer_index], preferred_element_type=jnp.float32) * inv_scale).astype(jnp.bfloat16)
        value_rows = (jnp.dot(scaled, w_value[layer_index], preferred_element_type=jnp.float32) * inv_scale).astype(jnp.bfloat16)
        outgate = (jnp.dot(scaled, w_outgate[layer_index], preferred_element_type=jnp.float32) * inv_scale).astype(jnp.bfloat16)
        gate_pre = jnp.dot(scaled, w_gates[layer_index], preferred_element_type=jnp.float32) * inv_scale
        input_pre = gate_pre[:, :HEADS] + gate_bias[layer_index, 0][None, :]
        forget_pre = gate_pre[:, HEADS:] + gate_bias[layer_index, 1][None, :]
        readout, new_memory, new_normalizer, new_max = cell_update(query, key_rows, value_rows, input_pre, forget_pre, memory[layer_index], normalizer[layer_index], stabilizer[layer_index])
        gated = (jax.nn.sigmoid(outgate.astype(jnp.float32)) * readout).astype(jnp.bfloat16)
        projected = jnp.dot(gated, w_out[layer_index], preferred_element_type=jnp.float32)
        current = (wide_rows + projected).astype(jnp.bfloat16)
        memories.append(new_memory)
        normalizers.append(new_normalizer)
        maxima.append(new_max)
    return (current, jnp.stack(memories), jnp.stack(normalizers), jnp.stack(maxima))
```

```python
import functools
import math

import jax
import jax.numpy as jnp
from jax import lax
from jax.experimental import pallas as pl
from jax.experimental.pallas import tpu as pltpu
from jax.sharding import PartitionSpec as P

HEAD = 128
ROWS = 8
EPS = 1e-06
MESH = pl.DeviceIdType.MESH
F32 = jnp.float32
BF16 = jnp.bfloat16


def ring_order(n):
    return sorted(range(1, n), key=lambda d: -min(d, n - d))


def plane_order(side):
    pairs = [(a, b) for a in range(side) for b in range(side) if a or b]
    return sorted(pairs, key=lambda t: -(min(t[0], side - t[0]) + min(t[1], side - t[1])))


def kernel(
    ntp,
    ndp,
    tok_h,
    gain_h,
    wq_h,
    wk_h,
    wv_h,
    wo_h,
    wg_h,
    bias_h,
    wout_h,
    mem_h,
    nrm_h,
    stab_h,
    mixed_o,
    mem_o,
    nrm_o,
    stab_o,
    tok_v,
    gain_v,
    w_v,
    wg_v,
    bias_v,
    wout_v,
    mem_v,
    memb_v,
    nrm_v,
    stab_v,
    xg,
    bsend,
    brecv,
    cg,
    dsend,
    drecv,
    small_sem,
    w_sem,
    wout_sem,
    mem_sem,
    out_sem,
    swap_sem,
    send_sem,
    recv_sem,
):
    nz = ntp // 2
    side = math.isqrt(ndp)
    width = ndp * 256
    all_heads = ntp
    tp = lax.axis_index("tp")
    dp = lax.axis_index("dp")
    z = tp // 2
    c = lax.rem(tp, 2)
    y = dp // side
    x = lax.rem(dp, side)

    def z_at(dz, flip):
        nc = 1 - c if flip else c
        return lax.rem(z + dz, nz) * 2 + nc

    def dp_at(dy, dx):
        return lax.rem(y + dy, side) * side + lax.rem(x + dx, side)

    partner = z * 2 + 1 - c
    z_near = [(dz, flip) for dz in ring_order(nz) for flip in (0, 1)]
    plane = plane_order(side)

    small = [
        pltpu.make_async_copy(tok_h, tok_v, small_sem.at[0]),
        pltpu.make_async_copy(gain_h, gain_v, small_sem.at[1]),
        pltpu.make_async_copy(wg_h, wg_v, small_sem.at[2]),
        pltpu.make_async_copy(bias_h, bias_v, small_sem.at[3]),
        pltpu.make_async_copy(nrm_h, nrm_v, small_sem.at[4]),
        pltpu.make_async_copy(stab_h, stab_v, small_sem.at[5]),
    ]
    for copy in small:
        copy.start()
    weights = []
    for i, ref in enumerate((wq_h, wk_h, wv_h, wo_h)):
        weights.append(
            pltpu.make_async_copy(ref, w_v.at[:, :, pl.ds(i * HEAD, HEAD)], w_sem.at[i])
        )
    for copy in weights:
        copy.start()
    own_out = wout_v.at[:, pl.ds(pl.multiple_of(c * HEAD, HEAD), HEAD)]
    load_out = pltpu.make_async_copy(wout_h, own_out, wout_sem)
    load_out.start()
    load_mem = pltpu.make_async_copy(mem_h, mem_v, mem_sem)
    load_mem.start()

    barrier = pltpu.get_barrier_semaphore()
    greeted = 0
    for dz, flip in z_near:
        pl.semaphore_signal(
            barrier, 1, device_id={"tp": z_at(dz, flip), "dp": dp}, device_id_type=MESH
        )
        greeted += 1
    for dy, dx in plane:
        for other in (tp, partner):
            pl.semaphore_signal(
                barrier, 1, device_id={"tp": other, "dp": dp_at(dy, dx)}, device_id_type=MESH
            )
            greeted += 1
    pl.semaphore_signal(barrier, 1, device_id={"tp": partner, "dp": dp}, device_id_type=MESH)
    greeted += 1

    for copy in small:
        copy.wait()
    row8 = lax.broadcasted_iota(jnp.int32, (1, ROWS, 128), 1)
    upper = row8 < 4
    lane = lax.broadcasted_iota(jnp.int32, (1, 128), 1)
    row_of = lax.broadcasted_iota(jnp.int32, (ROWS, 128), 0)

    wide = tok_v[...].astype(F32)
    own_x = jnp.concatenate([wide[:, :128], wide[:, 128:]], axis=0)
    xg[0, tp] = own_x.astype(BF16)

    source = lax.broadcasted_iota(jnp.int32, (2 * all_heads, 128), 0)
    target = lax.broadcasted_iota(jnp.int32, (2 * all_heads, 128), 1)
    pick = ((target == 0) & (source == tp)) | ((target == 1) & (source == all_heads + tp))
    one_hot = jnp.where(pick, 1.0, 0.0).astype(BF16)
    for layer in range(2):
        w_v[layer, :, 4 * HEAD :] = jnp.dot(
            wg_v[layer], one_hot, preferred_element_type=F32
        ).astype(BF16)
    load_out.wait()
    load_mem.wait()
    for copy in weights:
        copy.wait()
    memb_v[...] = mem_v[...].astype(BF16)

    pl.semaphore_wait(barrier, greeted)

    def send(src, dst, layer, phase, to_tp, to_dp):
        pltpu.make_async_remote_copy(
            src_ref=src,
            dst_ref=dst,
            send_sem=send_sem.at[layer, phase],
            recv_sem=recv_sem.at[layer, phase],
            device_id={"tp": to_tp, "dp": to_dp},
            device_id_type=MESH,
        ).start()

    def all_of(ref, sem):
        pltpu.make_async_copy(ref, ref, sem).wait()

    def share_x(layer):
        for dz, flip in z_near:
            send(xg.at[layer, tp], xg.at[layer, tp], layer, 0, z_at(dz, flip), dp)
        send(xg.at[layer, tp], xg.at[layer, tp], layer, 0, partner, dp)

    share_x(0)
    swap = pltpu.make_async_remote_copy(
        src_ref=own_out,
        dst_ref=own_out,
        send_sem=swap_sem.at[0],
        recv_sem=swap_sem.at[1],
        device_id={"tp": partner, "dp": dp},
        device_id_type=MESH,
    )
    swap.start()

    for layer in range(2):
        all_of(xg.at[layer, pl.ds(0, ntp - 1)], recv_sem.at[layer, 0])
        tiles = xg[layer].astype(F32).reshape(nz, 2, ROWS, 128)
        even, odd = tiles[:, 0], tiles[:, 1]
        low = jnp.where(upper, even, pltpu.roll(odd, 4, 1)).reshape(nz * ROWS, 128)
        high = jnp.where(upper, pltpu.roll(even, 4, 1), odd).reshape(nz * ROWS, 128)
        squares = jnp.sum(low * low + high * high, axis=1, keepdims=True)
        gain = gain_v[pl.ds(layer, 1), :].astype(F32)
        scaled = jnp.concatenate(
            [(low * gain[:, :128]).astype(BF16), (high * gain[:, 128:]).astype(BF16)], axis=1
        )
        terms = jnp.dot(scaled, w_v[layer], preferred_element_type=F32)
        gates = jnp.where(lane == 2, squares, terms[:, 4 * HEAD :])
        gates_high = gates.astype(BF16).astype(F32)
        gates_low = pltpu.roll(gates - gates_high, 3, 1)
        gates = jnp.where(lane < 3, gates_high, gates_low)
        bsend[layer] = (
            jnp.concatenate([terms[:, : 4 * HEAD], gates], axis=1)
            .astype(BF16)
            .reshape(ndp, ROWS, 5 * HEAD)
        )
        for dy, dx in plane:
            to = dp_at(dy, dx)
            send(bsend.at[layer, to], brecv.at[layer, dp], layer, 1, tp, to)
        brecv[layer, dp] = bsend[layer, dp]
        all_of(brecv.at[layer, pl.ds(0, ndp - 1)], recv_sem.at[layer, 1])

        sums = jnp.sum(brecv[layer].astype(F32), axis=0)
        extra = sums[:, 4 * HEAD :]
        extra = extra + pltpu.roll(extra, 125, 1)
        inv = lax.rsqrt(extra[:, 2:3] / width + EPS)
        query = (sums[:, :HEAD] * inv).astype(BF16)
        key = (sums[:, HEAD : 2 * HEAD] * inv).astype(BF16).astype(F32) * HEAD**-0.5
        value = (sums[:, 2 * HEAD : 3 * HEAD] * inv).astype(BF16).astype(F32)
        outgate = (sums[:, 3 * HEAD : 4 * HEAD] * inv).astype(BF16).astype(F32)
        input_pre = extra[:, 0:1] * inv + bias_v[layer, 0:1, :]
        forget_pre = extra[:, 1:2] * inv + bias_v[layer, 1:2, :]
        log_forget = jnp.minimum(forget_pre, 0.0) - jnp.log1p(jnp.exp(-jnp.abs(forget_pre)))
        carried = log_forget + stab_v[layer]
        new_max = jnp.maximum(carried, input_pre)
        keep = jnp.exp(carried - new_max)
        write = jnp.exp(input_pre - new_max)
        query_float = query.astype(F32)
        read = jnp.zeros((ROWS, HEAD), F32)
        for s in range(ROWS):
            one = jnp.where(row_of == s, query_float, 0.0).astype(BF16)
            read = read + lax.dot_general(
                one, memb_v[layer, s], (((1,), (1,)), ((), ())), preferred_element_type=F32
            )
        match = jnp.sum(key * query_float, axis=1, keepdims=True)
        numerator = keep * read + (write * match) * value
        normalizer = keep * nrm_v[layer] + write * key
        denominator = jnp.sum(normalizer * query_float, axis=1, keepdims=True)
        floor = jnp.maximum(jnp.maximum(jnp.abs(denominator), jnp.exp(-new_max)), 1.0)
        gated = (jax.nn.sigmoid(outgate) * (numerator / floor)).astype(BF16)
        slot = c * ndp + dp
        cg[layer, slot] = gated
        for dy, dx in plane:
            for other in (tp, partner):
                send(cg.at[layer, slot], cg.at[layer, slot], layer, 2, other, dp_at(dy, dx))
        send(cg.at[layer, slot], cg.at[layer, slot], layer, 2, partner, dp)

        nrm_v[layer] = normalizer
        stab_v[layer] = new_max
        value_columns = jnp.transpose(write * value)
        for s in range(ROWS):
            mem_v[layer, s] = (
                keep[s : s + 1, :] * mem_v[layer, s]
                + value_columns[:, s : s + 1] * key[s : s + 1, :]
            )
        pltpu.make_async_copy(mem_v.at[layer], mem_o.at[layer], out_sem.at[layer]).start()

        all_of(cg.at[layer, pl.ds(0, ntp - 1)], recv_sem.at[layer, 2])
        if layer == 0:
            swap.wait()
        heads = cg[layer].reshape(2, ndp * ROWS, 128)
        both = jnp.concatenate([heads[0], heads[1]], axis=1)
        product = jnp.dot(both, wout_v[layer], preferred_element_type=F32)
        left = product[:, :128].reshape(ndp, ROWS, 128)
        right = product[:, 128:].reshape(ndp, ROWS, 128)
        for_even = jnp.where(upper, left, pltpu.roll(right, 4, 1))
        for_odd = jnp.where(upper, pltpu.roll(left, 4, 1), right)
        mine = jnp.where(c == 0, for_even, for_odd)
        dsend[layer] = mine.astype(BF16)
        for dz in ring_order(nz):
            to = lax.rem(z + dz, nz)
            send(dsend.at[layer, to], drecv.at[layer, z], layer, 3, to * 2 + c, dp)
        drecv[layer, z] = dsend[layer, z]
        all_of(drecv.at[layer, pl.ds(0, nz - 1)], recv_sem.at[layer, 3])
        own_x = (own_x + jnp.sum(drecv[layer].astype(F32), axis=0)).astype(BF16)
        if layer == 0:
            xg[1, tp] = own_x
            own_x = own_x.astype(F32)
            share_x(1)

    wide = own_x.astype(F32)
    tok_v[...] = jnp.concatenate([wide[:4], wide[4:]], axis=1).astype(BF16)
    outs = [
        pltpu.make_async_copy(tok_v, mixed_o, small_sem.at[0]),
        pltpu.make_async_copy(nrm_v, nrm_o, small_sem.at[1]),
        pltpu.make_async_copy(stab_v, stab_o, small_sem.at[2]),
    ]
    for copy in outs:
        copy.start()
    for layer in range(2):
        all_of(xg.at[layer, pl.ds(0, ntp - 1)], send_sem.at[layer, 0])
        all_of(brecv.at[layer, pl.ds(0, ndp - 1)], send_sem.at[layer, 1])
        all_of(cg.at[layer, pl.ds(0, ntp - 1)], send_sem.at[layer, 2])
        all_of(drecv.at[layer, pl.ds(0, nz - 1)], send_sem.at[layer, 3])
        pltpu.make_async_copy(mem_v.at[layer], mem_o.at[layer], out_sem.at[layer]).wait()
    for copy in outs:
        copy.wait()


def body(ntp, ndp, *args):
    tokens, gain, wq, wk, wv, wo, wg, bias, wout, memory, normalizer, stabilizer = args
    nz = ntp // 2
    hbm = pl.BlockSpec(memory_space=pltpu.HBM)
    memory = memory.reshape(2, ROWS, HEAD, HEAD)
    normalizer = normalizer.reshape(2, ROWS, HEAD)
    out = pl.pallas_call(
        functools.partial(kernel, ntp, ndp),
        out_shape=(
            jax.ShapeDtypeStruct(tokens.shape, BF16),
            jax.ShapeDtypeStruct(memory.shape, F32),
            jax.ShapeDtypeStruct(normalizer.shape, F32),
            jax.ShapeDtypeStruct(stabilizer.shape, F32),
        ),
        in_specs=[hbm] * 12,
        out_specs=(hbm,) * 4,
        scratch_shapes=[
            pltpu.VMEM(tokens.shape, BF16),
            pltpu.VMEM(gain.shape, BF16),
            pltpu.VMEM((2, 256, 5 * HEAD), BF16),
            pltpu.VMEM(wg.shape, BF16),
            pltpu.VMEM(bias.shape, F32),
            pltpu.VMEM((2, 2 * HEAD, 256), BF16),
            pltpu.VMEM(memory.shape, F32),
            pltpu.VMEM(memory.shape, BF16),
            pltpu.VMEM(normalizer.shape, F32),
            pltpu.VMEM(stabilizer.shape, F32),
            pltpu.VMEM((2, ntp, ROWS, 128), BF16),
            pltpu.VMEM((2, ndp, ROWS, 5 * HEAD), BF16),
            pltpu.VMEM((2, ndp, ROWS, 5 * HEAD), BF16),
            pltpu.VMEM((2, 2 * ndp, ROWS, 128), BF16),
            pltpu.VMEM((2, nz, ROWS, 128), BF16),
            pltpu.VMEM((2, nz, ROWS, 128), BF16),
            pltpu.SemaphoreType.DMA((6,)),
            pltpu.SemaphoreType.DMA((4,)),
            pltpu.SemaphoreType.DMA,
            pltpu.SemaphoreType.DMA,
            pltpu.SemaphoreType.DMA((2,)),
            pltpu.SemaphoreType.DMA((2,)),
            pltpu.SemaphoreType.DMA((2, 4)),
            pltpu.SemaphoreType.DMA((2, 4)),
        ],
        compiler_params=pltpu.CompilerParams(collective_id=0, has_side_effects=True),
    )(tokens, gain, wq, wk, wv, wo, wg, bias, wout, memory, normalizer, stabilizer)
    mixed, new_memory, new_normalizer, new_stabilizer = out
    return (
        mixed,
        new_memory.reshape(2, ROWS, 1, HEAD, HEAD),
        new_normalizer.reshape(2, ROWS, 1, HEAD),
        new_stabilizer,
    )


def solution(mesh):
    placed = (
        P("tp", "dp"),
        P(None, "dp"),
        P(None, "dp", "tp"),
        P(None, "dp", "tp"),
        P(None, "dp", "tp"),
        P(None, "dp", "tp"),
        P(None, "dp", None),
        P(None, None, "tp"),
        P(None, "tp", "dp"),
        P(None, "dp", "tp", None, None),
        P(None, "dp", "tp", None),
        P(None, "dp", "tp"),
    )
    return jax.shard_map(
        functools.partial(body, mesh.shape["tp"], mesh.shape["dp"]),
        mesh=mesh,
        in_specs=placed,
        out_specs=(
            P("tp", "dp"),
            P(None, "dp", "tp", None, None),
            P(None, "dp", "tp", None),
            P(None, "dp", "tp"),
        ),
        check_vma=False,
    )
```

```python
import functools
import math

import jax
import jax.numpy as jnp
from jax import lax
from jax.experimental import pallas as pl
from jax.experimental.pallas import tpu as pltpu
from jax.sharding import PartitionSpec as P

HEAD = 128
ROWS = 8
EPS = 1e-06
GROUPS = ((0, 1), (1, 2), (2, 4), (4, 16))
MESH = pl.DeviceIdType.MESH
F32 = jnp.float32
BF16 = jnp.bfloat16


def ring_order(n):
    return sorted(range(1, n), key=lambda d: -min(d, n - d))


def plane_order(side):
    pairs = [(a, b) for a in range(side) for b in range(side) if a or b]
    return sorted(pairs, key=lambda t: -(min(t[0], side - t[0]) + min(t[1], side - t[1])))


def kernel(
    ntp,
    ndp,
    tok_h,
    gain_h,
    wq_h,
    wk_h,
    wv_h,
    wo_h,
    wg_h,
    bias_h,
    wout_h,
    mem_h,
    nrm_h,
    stab_h,
    mixed_o,
    mem_o,
    nrm_o,
    stab_o,
    tok_v,
    gain_v,
    w_v,
    wg_v,
    bias_v,
    wout_v,
    mem_v,
    memb_v,
    nrm_v,
    stab_v,
    xg,
    x1g,
    bsend,
    brecv,
    cg,
    dsend,
    drecv,
    last_send,
    last_recv,
    small_sem,
    w_sem,
    wout_sem,
    mem_sem,
    swap_sem,
    send_sem,
    recv_sem,
    group_sem,
):
    nz = ntp // 2
    side = math.isqrt(ndp)
    width = ndp * 256
    all_heads = ntp
    tp = lax.axis_index("tp")
    dp = lax.axis_index("dp")
    z = tp // 2
    c = lax.rem(tp, 2)
    y = dp // side
    x = lax.rem(dp, side)

    def z_at(dz, flip):
        nc = 1 - c if flip else c
        return lax.rem(z + dz, nz) * 2 + nc

    def dp_at(dy, dx):
        return lax.rem(y + dy, side) * side + lax.rem(x + dx, side)

    partner = z * 2 + 1 - c
    z_near = [(dz, flip) for dz in ring_order(nz) for flip in (0, 1)]
    plane = plane_order(side)

    small = [
        pltpu.make_async_copy(tok_h, tok_v, small_sem.at[0]),
        pltpu.make_async_copy(gain_h, gain_v, small_sem.at[1]),
        pltpu.make_async_copy(wg_h, wg_v, small_sem.at[2]),
        pltpu.make_async_copy(bias_h, bias_v, small_sem.at[3]),
        pltpu.make_async_copy(nrm_h, nrm_v, small_sem.at[4]),
        pltpu.make_async_copy(stab_h, stab_v, small_sem.at[5]),
    ]
    for copy in small:
        copy.start()
    weights = []
    for i, ref in enumerate((wq_h, wk_h, wv_h, wo_h)):
        weights.append(
            pltpu.make_async_copy(ref, w_v.at[:, :, pl.ds(i * HEAD, HEAD)], w_sem.at[i])
        )
    for copy in weights:
        copy.start()
    own_out = wout_v.at[:, pl.ds(pl.multiple_of(c * HEAD, HEAD), HEAD)]
    load_out = pltpu.make_async_copy(wout_h, own_out, wout_sem)
    load_out.start()
    load_mem = pltpu.make_async_copy(mem_h, mem_v, mem_sem)
    load_mem.start()

    barrier = pltpu.get_barrier_semaphore()
    greeted = 0
    for dz, flip in z_near:
        pl.semaphore_signal(
            barrier, 1, device_id={"tp": z_at(dz, flip), "dp": dp}, device_id_type=MESH
        )
        greeted += 1
    for dy, dx in plane:
        for other in (tp, partner):
            pl.semaphore_signal(
                barrier, 1, device_id={"tp": other, "dp": dp_at(dy, dx)}, device_id_type=MESH
            )
            greeted += 1
    pl.semaphore_signal(barrier, 1, device_id={"tp": partner, "dp": dp}, device_id_type=MESH)
    greeted += 1

    row8 = lax.broadcasted_iota(jnp.int32, (1, ROWS, 128), 1)
    upper = row8 < 4
    lane = lax.broadcasted_iota(jnp.int32, (1, 128), 1)
    row_of = lax.broadcasted_iota(jnp.int32, (ROWS, 128), 0)
    diagonal = lax.broadcasted_iota(jnp.int32, (ROWS, ROWS), 0) == lax.broadcasted_iota(
        jnp.int32, (ROWS, ROWS), 1
    )

    small[0].wait()
    wide = tok_v[...].astype(F32)
    own_x = jnp.concatenate([wide[:, :128], wide[:, 128:]], axis=0)
    xg[tp] = own_x.astype(BF16)
    pl.semaphore_wait(barrier, greeted)

    def send(src, dst, layer, phase, to_tp, to_dp, arrival=None):
        pltpu.make_async_remote_copy(
            src_ref=src,
            dst_ref=dst,
            send_sem=send_sem.at[layer, phase],
            recv_sem=recv_sem.at[layer, phase] if arrival is None else arrival,
            device_id={"tp": to_tp, "dp": to_dp},
            device_id_type=MESH,
        ).start()

    def all_of(ref, sem):
        pltpu.make_async_copy(ref, ref, sem).wait()

    for dz, flip in z_near:
        send(xg.at[tp], xg.at[tp], 0, 0, z_at(dz, flip), dp)
    send(xg.at[tp], xg.at[tp], 0, 0, partner, dp)
    load_out.wait()
    swap = pltpu.make_async_remote_copy(
        src_ref=own_out,
        dst_ref=own_out,
        send_sem=swap_sem.at[0],
        recv_sem=swap_sem.at[1],
        device_id={"tp": partner, "dp": dp},
        device_id_type=MESH,
    )
    swap.start()

    for copy in small[1:]:
        copy.wait()
    for copy in weights:
        copy.wait()
    source = lax.broadcasted_iota(jnp.int32, (2 * all_heads, 128), 0)
    target = lax.broadcasted_iota(jnp.int32, (2 * all_heads, 128), 1)
    pick = ((target == 0) & (source == tp)) | ((target == 1) & (source == all_heads + tp))
    one_hot = jnp.where(pick, 1.0, 0.0).astype(BF16)
    for layer in range(2):
        w_v[layer, :, 4 * HEAD :] = lax.dot_general(
            wg_v[layer], one_hot, (((0,), (0,)), ((), ())), preferred_element_type=F32
        ).astype(BF16)
    load_mem.wait()
    memb_v[...] = mem_v[...].astype(BF16)
    stab_columns = [
        jnp.sum(jnp.where(diagonal, stab_v[layer], 0.0), axis=1, keepdims=True)
        for layer in range(2)
    ]

    for layer in range(2):
        if layer == 0:
            all_of(xg.at[pl.ds(0, ntp - 1)], recv_sem.at[0, 0])
            tiles = xg[...].astype(F32).reshape(nz, 2, ROWS, 128)
            even, odd = tiles[:, 0], tiles[:, 1]
        else:
            all_of(drecv.at[pl.ds(0, nz - 1)], recv_sem.at[1, 0])
            tiles = x1g[...].astype(F32)
            even, odd = (
                jnp.concatenate([tiles[:, core, 0], tiles[:, core, 1]], axis=0) for core in (0, 1)
            )
        low = jnp.where(upper, even, pltpu.roll(odd, 4, 1)).reshape(nz * ROWS, 128)
        high = jnp.where(upper, pltpu.roll(even, 4, 1), odd).reshape(nz * ROWS, 128)
        squares = jnp.sum(low * low + high * high, axis=1, keepdims=True)
        gain = gain_v[pl.ds(layer, 1), :].astype(F32)
        scaled = jnp.concatenate(
            [(low * gain[:, :128]).astype(BF16), (high * gain[:, 128:]).astype(BF16)], axis=1
        )
        terms = jnp.dot(scaled, w_v[layer], preferred_element_type=F32)
        gates = jnp.where(lane == 2, squares, terms[:, 4 * HEAD :])
        gates_high = gates.astype(BF16).astype(F32)
        gates_low = pltpu.roll(gates - gates_high, 3, 1)
        gates = jnp.where(lane < 3, gates_high, gates_low)
        bsend[layer] = (
            jnp.concatenate([terms[:, : 4 * HEAD], gates], axis=1)
            .astype(BF16)
            .reshape(ndp, ROWS, 5 * HEAD)
        )
        for dy, dx in plane:
            to = dp_at(dy, dx)
            send(bsend.at[layer, to], brecv.at[layer, dp], layer, 1, tp, to)
        brecv[layer, dp] = bsend[layer, dp]
        all_of(brecv.at[layer, pl.ds(0, ndp - 1)], recv_sem.at[layer, 1])

        sums = jnp.sum(brecv[layer].astype(F32), axis=0)
        extra = sums[:, 4 * HEAD :]
        extra = extra + pltpu.roll(extra, 125, 1)
        inv = lax.rsqrt(extra[:, 2:3] / width + EPS)
        query = (sums[:, :HEAD] * inv).astype(BF16)
        key = (sums[:, HEAD : 2 * HEAD] * inv).astype(BF16).astype(F32) * HEAD**-0.5
        value = (sums[:, 2 * HEAD : 3 * HEAD] * inv).astype(BF16).astype(F32)
        outgate = (sums[:, 3 * HEAD : 4 * HEAD] * inv).astype(BF16).astype(F32)
        input_pre = extra[:, 0:1] * inv + bias_v[layer, :, 0:1]
        forget_pre = extra[:, 1:2] * inv + bias_v[layer, :, 1:2]
        log_forget = jnp.minimum(forget_pre, 0.0) - jnp.log1p(jnp.exp(-jnp.abs(forget_pre)))
        carried = log_forget + stab_columns[layer]
        new_max = jnp.maximum(carried, input_pre)
        keep = jnp.exp(carried - new_max)
        write = jnp.exp(input_pre - new_max)
        query_float = query.astype(F32)
        read = jnp.zeros((ROWS, HEAD), F32)
        for s in range(ROWS):
            one = jnp.where(row_of == s, query_float, 0.0).astype(BF16)
            read = read + lax.dot_general(
                one, memb_v[layer, s], (((1,), (1,)), ((), ())), preferred_element_type=F32
            )
        match = jnp.sum(key * query_float, axis=1, keepdims=True)
        numerator = keep * read + (write * match) * value
        normalizer = keep * nrm_v[layer] + write * key
        denominator = jnp.sum(normalizer * query_float, axis=1, keepdims=True)
        floor = jnp.maximum(jnp.maximum(jnp.abs(denominator), jnp.exp(-new_max)), 1.0)
        gated = (jax.nn.sigmoid(outgate) * (numerator / floor)).astype(BF16)
        slot = c * ndp + dp
        cg[layer, slot] = gated
        arrival = None
        if layer == 1:
            group = sum(jnp.where(dp >= first, 1, 0) for first, _ in GROUPS[1:])
            arrival = group_sem.at[group]
        for dy, dx in plane:
            for other in (tp, partner):
                to = dp_at(dy, dx)
                send(cg.at[layer, slot], cg.at[layer, slot], layer, 2, other, to, arrival)
        send(cg.at[layer, slot], cg.at[layer, slot], layer, 2, partner, dp, arrival)

        nrm_o[layer] = normalizer
        stab_o[layer] = jnp.sum(jnp.where(diagonal, new_max, 0.0), axis=0, keepdims=True)
        value_columns = jnp.transpose(write * value)
        for s in range(ROWS):
            mem_o[layer, s] = (
                keep[s : s + 1, :] * mem_v[layer, s]
                + value_columns[:, s : s + 1] * key[s : s + 1, :]
            )

        def projected(first, last):
            count = last - first
            heads = [
                cg[layer, pl.ds(core * ndp + first, count)].reshape(count * ROWS, 128)
                for core in (0, 1)
            ]
            both = jnp.concatenate(heads, axis=1)
            product = jnp.dot(both, wout_v[layer], preferred_element_type=F32)
            left = product[:, :128].reshape(count, ROWS, 128)
            right = product[:, 128:].reshape(count, ROWS, 128)
            for_even = jnp.where(upper, left, pltpu.roll(right, 4, 1))
            for_odd = jnp.where(upper, pltpu.roll(left, 4, 1), right)
            return jnp.where(c == 0, for_even, for_odd).astype(BF16)

        half = nz // 2
        if layer == 0:
            all_of(cg.at[layer, pl.ds(0, ntp - 1)], recv_sem.at[layer, 2])
            swap.wait()
            mine = projected(0, ndp)
            dsend[:, 0] = mine[:half]
            dsend[:, 1] = mine[half:]
            pair = lax.rem(z, half)
            for dz in ring_order(nz):
                to = lax.rem(z + dz, nz)
                send(dsend.at[lax.rem(to, half)], drecv.at[z], 0, 3, to * 2 + c, dp)
            drecv[z] = dsend[pair]
            before = jnp.stack([xg[2 * pair + c], xg[2 * (pair + half) + c]]).astype(F32)
            all_of(drecv.at[pl.ds(0, nz - 1)], recv_sem.at[0, 3])
            x1g[pair, c] = (before + jnp.sum(drecv[...].astype(F32), axis=0)).astype(BF16)
            mine_at = x1g.at[pair, c]
            for dz in sorted(range(1 - nz // 4, nz // 4 + 1), key=lambda d: -abs(d)):
                for flip in (0, 1):
                    if dz or flip:
                        send(mine_at, mine_at, 1, 0, z_at(dz + nz, flip), dp)
            own_x = x1g[pair, c, z // half].astype(F32)
        else:
            for index, (first, last) in enumerate(GROUPS):
                count = 2 * (last - first)
                inside = (dp >= first) & (dp < last)

                @pl.when(inside)
                def _():
                    all_of(cg.at[1, pl.ds(0, count - 1)], group_sem.at[index])

                @pl.when(jnp.logical_not(inside))
                def _():
                    all_of(cg.at[1, pl.ds(0, count)], group_sem.at[index])

                last_send[first:last] = projected(first, last)
                for to in range(first, last):

                    @pl.when(z != to)
                    def _():
                        send(last_send.at[to], last_recv.at[z], 1, 3, to * 2 + c, dp)

            last_recv[z] = last_send[z]
            all_of(last_recv.at[pl.ds(0, nz - 1)], recv_sem.at[1, 3])
            own_x = (own_x + jnp.sum(last_recv[...].astype(F32), axis=0)).astype(BF16)

    wide = own_x.astype(F32)
    mixed_o[...] = jnp.concatenate([wide[:4], wide[4:]], axis=1).astype(BF16)
    all_of(xg.at[pl.ds(0, ntp - 1)], send_sem.at[0, 0])
    all_of(drecv.at[pl.ds(0, nz - 1)], send_sem.at[1, 0])
    all_of(drecv.at[pl.ds(0, nz - 1)], send_sem.at[0, 3])
    all_of(last_recv.at[pl.ds(0, nz - 1)], send_sem.at[1, 3])
    for layer in range(2):
        all_of(brecv.at[layer, pl.ds(0, ndp - 1)], send_sem.at[layer, 1])
        all_of(cg.at[layer, pl.ds(0, ntp - 1)], send_sem.at[layer, 2])


def put_out(mixed_v, mem_v, nrm_v, stab_v, mixed_o, mem_o, nrm_o, stab_o, sem):
    copies = [
        pltpu.make_async_copy(mem_v, mem_o, sem.at[0]),
        pltpu.make_async_copy(nrm_v, nrm_o, sem.at[1]),
        pltpu.make_async_copy(stab_v, stab_o, sem.at[2]),
        pltpu.make_async_copy(mixed_v, mixed_o, sem.at[3]),
    ]
    for copy in copies:
        copy.start()
    for copy in copies:
        copy.wait()


def body(ntp, ndp, *args):
    tokens, gain, wq, wk, wv, wo, wg, bias, wout, memory, normalizer, stabilizer = args
    nz = ntp // 2
    hbm = pl.BlockSpec(memory_space=pltpu.HBM)
    memory = memory.reshape(2, ROWS, HEAD, HEAD)
    normalizer = normalizer.reshape(2, ROWS, HEAD)
    wg = jnp.transpose(wg, (0, 2, 1))
    bias = jnp.transpose(bias, (0, 2, 1))
    stabilizer = jnp.transpose(stabilizer, (0, 2, 1))
    out = pl.pallas_call(
        functools.partial(kernel, ntp, ndp),
        out_shape=(
            pltpu.VMEM(tokens.shape, BF16),
            pltpu.VMEM(memory.shape, F32),
            pltpu.VMEM(normalizer.shape, F32),
            pltpu.VMEM(stabilizer.shape, F32),
        ),
        in_specs=[hbm] * 12,
        out_specs=(pl.BlockSpec(memory_space=pltpu.VMEM),) * 4,
        scratch_shapes=[
            pltpu.VMEM(tokens.shape, BF16),
            pltpu.VMEM(gain.shape, BF16),
            pltpu.VMEM((2, 256, 5 * HEAD), BF16),
            pltpu.VMEM(wg.shape, BF16),
            pltpu.VMEM(bias.shape, F32),
            pltpu.VMEM((2, 2 * HEAD, 256), BF16),
            pltpu.VMEM(memory.shape, F32),
            pltpu.VMEM(memory.shape, BF16),
            pltpu.VMEM(normalizer.shape, F32),
            pltpu.VMEM(stabilizer.shape, F32),
            pltpu.VMEM((ntp, ROWS, 128), BF16),
            pltpu.VMEM((nz // 2, 2, 2, ROWS, 128), BF16),
            pltpu.VMEM((2, ndp, ROWS, 5 * HEAD), BF16),
            pltpu.VMEM((2, ndp, ROWS, 5 * HEAD), BF16),
            pltpu.VMEM((2, 2 * ndp, ROWS, 128), BF16),
            pltpu.VMEM((nz // 2, 2, ROWS, 128), BF16),
            pltpu.VMEM((nz, 2, ROWS, 128), BF16),
            pltpu.VMEM((nz, ROWS, 128), BF16),
            pltpu.VMEM((nz, ROWS, 128), BF16),
            pltpu.SemaphoreType.DMA((6,)),
            pltpu.SemaphoreType.DMA((4,)),
            pltpu.SemaphoreType.DMA,
            pltpu.SemaphoreType.DMA,
            pltpu.SemaphoreType.DMA((2,)),
            pltpu.SemaphoreType.DMA((2, 4)),
            pltpu.SemaphoreType.DMA((2, 4)),
            pltpu.SemaphoreType.DMA((len(GROUPS),)),
        ],
        compiler_params=pltpu.CompilerParams(collective_id=0, has_side_effects=True),
    )(tokens, gain, wq, wk, wv, wo, wg, bias, wout, memory, normalizer, stabilizer)
    mixed, new_memory, new_normalizer, new_stabilizer = pl.pallas_call(
        put_out,
        out_shape=tuple(jax.ShapeDtypeStruct(o.shape, o.dtype) for o in out),
        in_specs=[pl.BlockSpec(memory_space=pltpu.VMEM)] * 4,
        out_specs=(hbm,) * 4,
        scratch_shapes=[pltpu.SemaphoreType.DMA((4,))],
    )(*(pltpu.with_memory_space_constraint(o, pltpu.VMEM) for o in out))
    return (
        mixed,
        new_memory.reshape(2, ROWS, 1, HEAD, HEAD),
        new_normalizer.reshape(2, ROWS, 1, HEAD),
        jnp.transpose(new_stabilizer, (0, 2, 1)),
    )


def solution(mesh):
    placed = (
        P("tp", "dp"),
        P(None, "dp"),
        P(None, "dp", "tp"),
        P(None, "dp", "tp"),
        P(None, "dp", "tp"),
        P(None, "dp", "tp"),
        P(None, "dp", None),
        P(None, None, "tp"),
        P(None, "tp", "dp"),
        P(None, "dp", "tp", None, None),
        P(None, "dp", "tp", None),
        P(None, "dp", "tp"),
    )
    return jax.shard_map(
        functools.partial(body, mesh.shape["tp"], mesh.shape["dp"]),
        mesh=mesh,
        in_specs=placed,
        out_specs=(
            P("tp", "dp"),
            P(None, "dp", "tp", None, None),
            P(None, "dp", "tp", None),
            P(None, "dp", "tp"),
        ),
        check_vma=False,
    )
```
